32 devices in a mesh: sp: 8 (over z, x), tp: 4 (over y, core).
Axes of the slice: x: 2, y: 2, z: 4, core: 2. Of those that a mesh axis runs over, the one named last changes fastest.
Arguments:
- out_gate: bfloat16 [4096, 1536], P('sp', 'tp'), may hold values from -6 to 6
- in_gate: bfloat16 [4096, 1536], P('sp', 'tp'), may hold values from -6 to 6
- conv_values: bfloat16 [4096, 1536], P('sp', 'tp'), may hold values from -6 to 6
- conv_taps: float32 [3, 1536], P(None, 'tp'), may hold values from -3 to 3
- mix_gain: float32 [1536], replicated, may hold values from 0.1 to 1.9
- out_proj: bfloat16 [1536, 2048], replicated, may hold values from -0.15625 to 0.15625
- residual: bfloat16 [4096, 2048], P(('sp', 'tp')), may hold values from -6 to 6
- ffn_gain: float32 [2048], replicated, may hold values from 0.1 to 1.9
- routes: int32 [4096, 6], P(('sp', 'tp')), may hold values from 0 to 31, all different within a row; in each aligned block of 128 rows (0 to 127, 128 to 255, ...) at most 32 rows name the same one
- route_weights: float32 [4096, 6], P(('sp', 'tp')), may hold values from 0.05 to 1
- shared_gate: bfloat16 [2048, 512], replicated, may hold values from -0.125 to 0.125
- shared_up: bfloat16 [2048, 512], replicated, may hold values from -0.125 to 0.125
- shared_down: bfloat16 [512, 2048], replicated, may hold values from -0.25 to 0.25
- expert_gate: bfloat16 [32, 2048, 512], P(('sp', 'tp')), may hold values from -0.125 to 0.125
- expert_up: bfloat16 [32, 2048, 512], P(('sp', 'tp')), may hold values from -0.125 to 0.125
- expert_down: bfloat16 [32, 512, 2048], P(('sp', 'tp')), may hold values from -0.25 to 0.25
Outputs:
- layer_out: bfloat16 [4096, 2048], P(('sp', 'tp'))
The draws below stay inside these ranges and needn't reach their ends.
Inputs may be any that keep to these rules, and one draw needn't show every extreme that they name: `routes`: each row names 6 different experts. Within the rows of one device (aligned blocks of 128 rows) no expert is named more than 32 times, a bound that some block reaches.
All inputs are finite; a program needn't handle non-finite values.
Results may differ from the reference program's by a relative error of at most 0.0065.
Values may be sent and summed in bfloat16 or wider, within the bound.
A program may use at most 128 MiB of HBM per device.

```python
import math
import jax
import jax.numpy as jnp
import numpy as np
from jax import lax

D = 2048
DC = 1536
KERNEL = 3
FF_E = 512
FS = 512
TOP = 6
ROWS_DEV = 128
TOKENS = 4096
EXPERTS = 32
CAP = 32
N_SP = 8
N_TP = 4


def levels(key, shape, shards, smallest, largest):
    level = 1.0
    for axis_at, parts in shards:
        steps = jax.random.uniform(jax.random.fold_in(jax.random.fold_in(key, 6), axis_at), (parts,), jnp.float32, smallest / len(shards), largest / len(shards))
        level = level * jnp.repeat(jnp.exp(steps), shape[axis_at] // parts).reshape((-1,) + (1,) * (len(shape) - 1 - axis_at))
    return level


def deal_out(stream_key, own, number, rows, number_of, top, limit, slope):
    order = jax.random.permutation(stream_key, number_of)
    packed, common = portions_of(number_of, rows * top, limit, slope, True), portions_of(number_of, rows * top, limit, slope, False)
    places = jnp.arange(number_of)

    def named(sizes, offset_by):
        used = int((sizes > 0).sum())
        fixed = max(1, used // 4)
        passed = fixed + (places - fixed + offset_by * (used - fixed)) % max(1, number_of - fixed)
        return jnp.zeros((number_of,), jnp.int32).at[order[jnp.where(places < fixed, places, passed)]].set(jnp.asarray(sizes, jnp.int32))

    sizes = jnp.where(number % 4 == 0, named(packed, number // 4), named(common, number - number // 4 - 1))
    mixed = jax.random.permutation(jax.random.fold_in(own, 3), number_of)
    source_of, taker = mixed[0:number_of // 2 * 2:2], mixed[1:number_of // 2 * 2:2]
    margin = jnp.minimum(sizes[source_of] - 1, limit - sizes[taker]) // 2
    margin = jnp.where((source_of == order[0]) | (taker == order[0]) | (sizes[taker] == 0), 0, jnp.maximum(margin, 0))
    passed = jax.random.randint(jax.random.fold_in(own, 4), (number_of // 2,), 0, 1 << 20) % (margin + 1)
    sizes = sizes.at[source_of].add(-passed).at[taker].add(passed)
    labels = jnp.searchsorted(jnp.cumsum(sizes), jnp.arange(rows * top), side="right").astype(jnp.int32)
    listing = labels.reshape(top, rows).T
    listing = listing[jax.random.permutation(jax.random.fold_in(own, 1), rows)]
    offset_by = jax.random.randint(jax.random.fold_in(own, 2), (rows, 1), 0, top)
    return jnp.take_along_axis(listing, (jnp.arange(top)[None, :] + offset_by) % top, axis=1)


def portions_of(count, total, reach, slope, full):
    portions = [(1 << 20) // math.isqrt(rank ** slope) + 1 for rank in range(1, count + 1)]
    largest = reach if full else min(reach, max(-(-total // count), total * portions[0] // sum(portions)))
    least = 1 if total - largest >= count - 1 else 0
    given, surplus = [largest] + [least] * (count - 1), total - largest - least * (count - 1)
    while surplus > 0:
        movable = [i for i in range(1, count) if given[i] < largest] or [i for i in range(1, count) if given[i] < reach]
        whole, remaining = sum([portions[i] for i in movable]), surplus
        for i in movable:
            addition = min(reach - given[i], max(1, remaining * portions[i] // whole), surplus)
            given[i] = given[i] + addition
            surplus = surplus - addition
    return np.array(given)


def gaussian(own_key, shape, deviation, limit, split=(), kind=jnp.bfloat16):
    values = jax.random.normal(own_key, shape, jnp.float32) * deviation
    if len(split) > 0:
        values = levels(own_key, shape, split, -0.22, 0.18) * values
    return jnp.clip(values, min=-limit, max=limit).astype(kind)


def setup_inputs(seed: int = 0) -> dict:
    splits = jax.random.split(jax.random.key(seed), 17)
    out_gate = gaussian(splits[0], (TOKENS, DC), 1.0, 6.0, ((0, 8), (1, 4)))
    in_gate = gaussian(splits[1], (TOKENS, DC), 1.0, 6.0, ((0, 8), (1, 4)))
    conv_values = gaussian(splits[2], (TOKENS, DC), 1.0, 6.0, ((0, 8), (1, 4)))
    conv_taps = gaussian(splits[3], (KERNEL, DC), 0.6, 3.0, ((1, 4),), jnp.float32)
    mix_gain = jnp.clip(1.0 + 0.18 * jax.random.normal(splits[4], (DC,), jnp.float32), 0.1, 1.9)
    out_proj = gaussian(splits[5], (DC, D), DC ** -0.5, 0.15625)
    residual = gaussian(splits[6], (TOKENS, D), 1.0, 6.0, ((0, 32),))
    ffn_gain = jnp.clip(1.0 + 0.18 * jax.random.normal(splits[7], (D,), jnp.float32), 0.1, 1.9)
    routes_keys = jax.random.split(jax.random.fold_in(splits[8], 1), TOKENS // ROWS_DEV)
    routes_turns = jax.random.permutation(jax.random.fold_in(splits[8], 3), TOKENS // ROWS_DEV)
    routes = jax.vmap(lambda own, number: deal_out(jax.random.fold_in(splits[8], 2), own, number, ROWS_DEV, EXPERTS, TOP, CAP, 2))(routes_keys, routes_turns).reshape((TOKENS, TOP))
    route_weights = jnp.clip(jnp.exp(math.log(1.0) - 2.9957323 * jax.random.uniform(splits[9], (TOKENS, TOP), jnp.float32) ** levels(splits[9], (TOKENS, TOP), ((0, 32),), -0.2, 0.2)), 0.05, 1.0)
    shared_gate = gaussian(splits[10], (D, FS), D ** -0.5, 0.125)
    shared_up = gaussian(splits[11], (D, FS), D ** -0.5, 0.125)
    shared_down = gaussian(splits[12], (FS, D), FS ** -0.5, 0.25)
    expert_gate = gaussian(splits[13], (EXPERTS, D, FF_E), D ** -0.5, 0.125, ((0, 32),))
    expert_up = gaussian(splits[14], (EXPERTS, D, FF_E), D ** -0.5, 0.125, ((0, 32),))
    expert_down = gaussian(splits[15], (EXPERTS, FF_E, D), FF_E ** -0.5, 0.25, ((0, 32),))
    return dict(out_gate=out_gate, in_gate=in_gate, conv_values=conv_values, conv_taps=conv_taps, mix_gain=mix_gain, out_proj=out_proj, residual=residual, ffn_gain=ffn_gain, routes=routes, route_weights=route_weights, shared_gate=shared_gate, shared_up=shared_up, shared_down=shared_down, expert_gate=expert_gate, expert_up=expert_up, expert_down=expert_down)


def project_norm(conv_out, mix_gain, out_proj):
    values = conv_out.astype(jnp.float32)
    inverse = lax.rsqrt(lax.optimization_barrier(jnp.mean(values * values, axis=-1)) + 1e-06)
    scaled = (values * mix_gain).astype(jnp.bfloat16)
    return jnp.dot(scaled, out_proj, preferred_element_type=jnp.float32) * inverse[:, None]

def ffn_input(stream, ffn_gain):
    inverse = lax.rsqrt(lax.optimization_barrier(jnp.mean(stream * stream, axis=-1, keepdims=True)) + 1e-06)
    return (stream * inverse * ffn_gain).astype(jnp.bfloat16)

def swiglu_hidden(row_block, weight_gate, weight_up):
    gate_part = jnp.dot(row_block, weight_gate, preferred_element_type=jnp.float32)
    up_part = jnp.dot(row_block, weight_up, preferred_element_type=jnp.float32)
    return (jax.nn.silu(gate_part) * up_part).astype(jnp.bfloat16)

def reference(out_gate, in_gate, conv_values, conv_taps, mix_gain, out_proj, residual, ffn_gain, routes, route_weights, shared_gate, shared_up, shared_down, expert_gate, expert_up, expert_down):
    mixed_in = in_gate.astype(jnp.float32) * conv_values.astype(jnp.float32)
    taps_count = conv_taps.shape[0]
    length = mixed_in.shape[0]
    extended = jnp.concatenate([jnp.zeros((taps_count - 1, mixed_in.shape[1]), jnp.float32), mixed_in], axis=0)
    filtered = conv_taps[0] * extended[0:length]
    for offset in range(1, taps_count):
        filtered = filtered + conv_taps[offset] * extended[offset:offset + length]
    conv_out = (out_gate.astype(jnp.float32) * filtered).astype(jnp.bfloat16)
    stream = residual.astype(jnp.float32) + project_norm(conv_out, mix_gain, out_proj)
    normed = ffn_input(stream, ffn_gain)
    shared_result = jnp.dot(swiglu_hidden(normed, shared_gate, shared_up), shared_down, preferred_element_type=jnp.float32)
    top_count = routes.shape[1]
    token_count = routes.shape[0]
    model_width = normed.shape[1]
    flat_ids = routes.reshape(-1).astype(jnp.int32)
    gate_values = route_weights / lax.optimization_barrier(jnp.sum(route_weights, axis=1, keepdims=True)) * 2.5
    flat_gates = gate_values.reshape(-1)
    sort_order = jnp.argsort(flat_ids, stable=True).astype(jnp.int32)
    sorted_ids = flat_ids[sort_order]
    counts = jnp.bincount(flat_ids, length=EXPERTS).astype(jnp.int32)
    starts = (jnp.cumsum(counts) - counts).astype(jnp.int32)
    slot_rank = jnp.arange(flat_ids.shape[0], dtype=jnp.int32) - starts[sorted_ids]
    most_rows = N_SP * N_TP * CAP
    slot_index = (sorted_ids * most_rows + slot_rank).astype(jnp.int32)
    row_of = (sort_order // top_count).astype(jnp.int32)
    slot_rows = jnp.full((EXPERTS * most_rows,), token_count, jnp.int32).at[slot_index].set(row_of)
    slot_gates = jnp.zeros((EXPERTS * most_rows,), jnp.float32).at[slot_index].set(flat_gates[sort_order])
    padded = jnp.concatenate([normed, jnp.zeros((1, model_width), jnp.bfloat16)], axis=0)

    def add_expert(running, inputs):
        row_index, gate_slots, weight_gate, weight_up, weight_down = inputs
        picked = padded[row_index]
        hidden = swiglu_hidden(picked, weight_gate, weight_up)
        result = jnp.dot(hidden, weight_down, preferred_element_type=jnp.float32).astype(jnp.bfloat16)
        return (running.at[row_index].add(result.astype(jnp.float32) * gate_slots[:, None]), None)
    running = jnp.zeros((token_count + 1, model_width), jnp.float32)
    running, _ = lax.scan(add_expert, running, (slot_rows.reshape(EXPERTS, most_rows), slot_gates.reshape(EXPERTS, most_rows), expert_gate, expert_up, expert_down))
    routed = running[:token_count]
    return (stream + shared_result + routed).astype(jnp.bfloat16)
```

```python
import functools

import jax
import jax.numpy as jnp
from jax import lax
from jax.experimental import pallas as pl
from jax.experimental.pallas import tpu as pltpu
from jax.sharding import PartitionSpec as P

MESH = pl.DeviceIdType.MESH
META_ROWS = 16


def from_behind(block, axis, distance):
    devices = range(lax.axis_size(axis))
    route = [(i - distance, i) for i in devices if i - distance in devices]
    return lax.ppermute(block, axis, route)


def project_norm(conv_out, mix_gain, out_proj):
    values = conv_out.astype(jnp.float32)
    inverse = lax.rsqrt(jnp.mean(values * values, axis=-1) + 1e-06)
    scaled = (values * mix_gain).astype(jnp.bfloat16)
    return jnp.dot(scaled, out_proj, preferred_element_type=jnp.float32) * inverse[:, None]


def ffn(x, gate, up, down):
    g = jnp.dot(x, gate[...], preferred_element_type=jnp.float32)
    u = jnp.dot(x, up[...], preferred_element_type=jnp.float32)
    h = (g / (1.0 + jnp.exp(-g)) * u).astype(jnp.bfloat16)
    return jnp.dot(h, down[...], preferred_element_type=jnp.float32)


def experts_kernel(
    n_sp, n_tp, width_x, cap, top,
    normed, stream, meta_own, eg_hbm, eu_hbm, ed_hbm, sg_hbm, su_hbm, sd_hbm,
    out,
    gathered, metas, staged, arrived, results, returned,
    left_in, right_in, left_out, right_out, total,
    eg, eu, ed, sg, su, sd,
    w_sem, meta_send, meta_recv, ring_send, ring_recv,
    disp_send, disp_recv, ret_send, ret_recv, red_send, red_recv,
):
    sp = lax.axis_index("sp")
    tp = lax.axis_index("tp")
    half = n_sp // 2
    rows = normed.shape[0]
    mid = rows // 2
    group = n_tp * cap
    width_z = n_sp // width_x

    def place_of(index):
        x, z = lax.rem(index, width_x), lax.div(index, width_x)
        return x * width_z + z + lax.rem(x, 2) * (width_z - 1 - 2 * z)

    def index_of(place):
        x, zz = lax.div(place, width_z), lax.rem(place, width_z)
        return (zz + lax.rem(x, 2) * (width_z - 1 - 2 * zz)) * width_x + x

    place = place_of(sp)

    def ahead(distance):
        return index_of(lax.rem(place + distance, n_sp))

    right, left = ahead(1), ahead(n_sp - 1)

    def partner(j):
        return lax.rem(tp + j, n_tp)

    barrier = pltpu.get_barrier_semaphore()
    for d in range(1, n_sp):
        pl.semaphore_signal(barrier, inc=1, device_id=(ahead(d), tp), device_id_type=MESH)
    for j in range(1, n_tp):
        pl.semaphore_signal(barrier, inc=1, device_id=(sp, partner(j)), device_id_type=MESH)

    weights = [
        pltpu.make_async_copy(src, dst, w_sem.at[i])
        for i, (src, dst) in enumerate(
            ((sg_hbm, sg), (su_hbm, su), (sd_hbm, sd),
             (eg_hbm.at[0], eg), (eu_hbm.at[0], eu), (ed_hbm.at[0], ed))
        )
    ]
    for copy in weights:
        copy.start()
    pl.semaphore_wait(barrier, n_sp - 1 + n_tp - 1)

    def remote(src, dst, send, recv, device):
        return pltpu.make_async_remote_copy(
            src_ref=src, dst_ref=dst, send_sem=send, recv_sem=recv,
            device_id=device, device_id_type=MESH,
        )

    def meta_copy(d):
        return remote(meta_own, metas.at[d], meta_send.at[d], meta_recv.at[d], (ahead(d), tp))

    def ring_copy(s, way, src=None):
        device = (right if way == 0 else left, tp)
        dst = gathered.at[s + 1 if way == 0 else n_sp - s - 1]
        if src is None:
            src = gathered.at[s if way == 0 else lax.rem(n_sp - s, n_sp)]
        return remote(src, dst, ring_send.at[way, s], ring_recv.at[way, s], device)

    def ring_half(way):
        device = (right if way == 0 else left, tp)
        part = pl.ds(0 if way == 0 else mid, mid)
        s = half - 1
        src = gathered.at[s if way == 0 else n_sp - s, part]
        return remote(src, gathered.at[half, part], ring_send.at[way, s], ring_recv.at[way, s], device)

    def disp_copy(d, j):
        src = staged.at[d, pl.ds(pl.multiple_of(partner(j) * cap, cap), cap)]
        dst = arrived.at[d, pl.ds(pl.multiple_of(tp * cap, cap), cap)]
        return remote(src, dst, disp_send.at[d, j], disp_recv.at[d, j], (sp, partner(j)))

    def ret_copy(d, j):
        src = results.at[d, pl.ds(pl.multiple_of(partner(j) * cap, cap), cap)]
        dst = returned.at[d, pl.ds(pl.multiple_of(tp * cap, cap), cap)]
        return remote(src, dst, ret_send.at[d, j], ret_recv.at[d, j], (sp, partner(j)))

    def red_copy(s, way):
        device = (left if way == 0 else right, tp)
        src = (left_out if way == 0 else right_out).at[s]
        dst = (left_in if way == 0 else right_in).at[s - 1]
        return remote(src, dst, red_send.at[way, s], red_recv.at[way, s - 1], device)

    def red_half(way):
        device = (left if way == 0 else right, tp)
        part = pl.ds(0 if way == 0 else mid, mid)
        src = (left_out if way == 0 else right_out).at[half, part]
        dst = (left_in if way == 0 else right_in).at[half - 1, part]
        return remote(src, dst, red_send.at[way, half], red_recv.at[way, half - 1], device)

    first_slot = (sp * group).astype(jnp.float32)

    def matches(meta, k):
        slots = lax.broadcasted_iota(jnp.int32, (group, rows), 0).astype(jnp.float32) + first_slot
        return slots == meta[k : k + 1, :]

    def dispatch(d, block, meta):
        pick = jnp.zeros((group, rows), jnp.float32)
        for k in range(top):
            pick = jnp.where(matches(meta, k), 1.0, pick)
        staged[d] = jnp.dot(
            pick.astype(jnp.bfloat16), block, preferred_element_type=jnp.float32
        ).astype(jnp.bfloat16)
        for j in range(1, n_tp):
            disp_copy(d, j).start()

    own = pl.ds(pl.multiple_of(tp * cap, cap), cap)

    def run_expert(d):
        for j in range(1, n_tp):
            disp_copy(d, j).wait_recv()
        arrived[d, own] = staged[d, own]
        results[d] = ffn(arrived[d], eg, eu, ed).astype(jnp.bfloat16)

    def combine(d, meta):
        for j in range(1, n_tp):
            ret_copy(d, j).wait_recv()
        returned[d, own] = results[d, own]
        mix = jnp.zeros((group, rows), jnp.float32)
        for k in range(top):
            mix = jnp.where(matches(meta, k), meta[top + k : top + k + 1, :], mix)
        return lax.dot_general(
            mix.astype(jnp.bfloat16), returned[d], (((0,), (0,)), ((), ())),
            preferred_element_type=jnp.float32,
        )

    ring_copy(0, 0, normed).start()
    ring_copy(0, 1, normed).start()
    for d in range(1, n_sp):
        meta_copy(d).start()
    dispatch(0, normed[...], meta_own[...])
    left_in[half - 1, mid:] = jnp.zeros((rows - mid, normed.shape[1]), jnp.bfloat16)
    right_in[half - 1, :mid] = jnp.zeros((mid, normed.shape[1]), jnp.bfloat16)
    for copy in weights[:3]:
        copy.wait()
    total[...] = stream[...] + ffn(normed[...], sg, su, sd)
    for copy in weights[3:]:
        copy.wait()

    def gather_step(s, carry):
        ring_copy(s - 1, 0).wait_recv()
        ring_copy(s - 1, 1).wait_recv()

        @pl.when(s < half - 1)
        def _():
            ring_copy(s, 0).start()
            ring_copy(s, 1).start()

        @pl.when(s == half - 1)
        def _():
            ring_half(0).start()
            ring_half(1).start()

        def one(i, c):
            d = s + i * (n_sp - 2 * s)
            meta_copy(d).wait_recv()
            dispatch(d, gathered[d], metas[d])
            return c

        lax.fori_loop(0, 2, one, 0)

        @pl.when(s == 1)
        def _():
            run_expert(0)

        @pl.when(s > 1)
        def _():
            def two(i, c):
                run_expert(s - 1 + i * (n_sp - 2 * (s - 1)))
                return c

            lax.fori_loop(0, 2, two, 0)

        return carry

    lax.fori_loop(1, half, gather_step, 0)
    ring_half(0).wait_recv()
    ring_half(1).wait_recv()
    meta_copy(half).wait_recv()
    dispatch(half, gathered[half], metas[half])

    def last(i, c):
        run_expert(jnp.where(i == 2, half, half - 1 + 2 * i))
        return c

    lax.fori_loop(0, 3, last, 0)

    def give_back(d):
        for j in range(1, n_tp):
            ret_copy(d, j).start()

    give_back(half)
    for s in range(half - 1, 0, -1):
        give_back(s)
        give_back(n_sp - s)
    give_back(0)

    part = combine(half, metas[half])
    left_out[half, :mid] = part[:mid].astype(jnp.bfloat16)
    right_out[half, mid:] = part[mid:].astype(jnp.bfloat16)
    red_half(0).start()
    red_half(1).start()

    def reduce_step(i, carry):
        s = half - 1 - i
        for way, (d, buf_in, buf_out) in enumerate(
            ((s, left_in, left_out), (n_sp - s, right_in, right_out))
        ):
            part = combine(d, metas[d])

            @pl.when(s == half - 1)
            def _():
                red_half(way).wait_recv()

            @pl.when(s < half - 1)
            def _():
                red_copy(s + 1, way).wait_recv()

            buf_out[s] = (part + buf_in[s].astype(jnp.float32)).astype(jnp.bfloat16)
            red_copy(s, way).start()
        return carry

    lax.fori_loop(0, half - 1, reduce_step, 0)
    part = combine(0, meta_own[...]) + total[...]
    for way, buf_in in enumerate((left_in, right_in)):
        red_copy(1, way).wait_recv()
        part = part + buf_in[0].astype(jnp.float32)
    out[...] = part.astype(out.dtype)

    for d in range(1, n_sp):
        meta_copy(d).wait_send()
    for way in range(2):
        ring_copy(0, way, normed).wait_send()
        for s in range(1, half - 1):
            ring_copy(s, way).wait_send()
        ring_half(way).wait_send()
        red_half(way).wait_send()
        for s in range(1, half):
            red_copy(s, way).wait_send()

    def drain(d, c):
        for j in range(1, n_tp):
            disp_copy(d, j).wait_send()
            ret_copy(d, j).wait_send()
        return c

    lax.fori_loop(0, n_sp, drain, 0)


def routed_and_shared(normed, stream, meta, cap, top, eg, eu, ed, sg, su, sd):
    n_sp, n_tp = lax.axis_size("sp"), lax.axis_size("tp")
    rows, width = normed.shape
    hidden, shared_hidden = eg.shape[-1], sg.shape[-1]
    half = n_sp // 2
    group = n_tp * cap
    width_x = max(1, n_tp // 2)
    if n_sp % width_x:
        width_x = 1
    bf, f32 = jnp.bfloat16, jnp.float32
    vmem = pl.BlockSpec(memory_space=pltpu.VMEM)
    anywhere = pl.BlockSpec(memory_space=pl.ANY)
    dma = pltpu.SemaphoreType.DMA
    return pl.pallas_call(
        functools.partial(experts_kernel, n_sp, n_tp, width_x, cap, top),
        out_shape=jax.ShapeDtypeStruct((rows, width), bf),
        in_specs=[vmem] * 3 + [anywhere] * 6,
        out_specs=vmem,
        scratch_shapes=[
            pltpu.VMEM((n_sp, rows, width), bf),
            pltpu.VMEM((n_sp, META_ROWS, rows), f32),
            pltpu.VMEM((n_sp, group, width), bf),
            pltpu.VMEM((n_sp, group, width), bf),
            pltpu.VMEM((n_sp, group, width), bf),
            pltpu.VMEM((n_sp, group, width), bf),
            pltpu.VMEM((half, rows, width), bf),
            pltpu.VMEM((half, rows, width), bf),
            pltpu.VMEM((half + 1, rows, width), bf),
            pltpu.VMEM((half + 1, rows, width), bf),
            pltpu.VMEM((rows, width), f32),
            pltpu.VMEM((width, hidden), bf),
            pltpu.VMEM((width, hidden), bf),
            pltpu.VMEM((hidden, width), bf),
            pltpu.VMEM((width, shared_hidden), bf),
            pltpu.VMEM((width, shared_hidden), bf),
            pltpu.VMEM((shared_hidden, width), bf),
            dma((6,)),
            dma((n_sp,)),
            dma((n_sp,)),
            dma((2, half)),
            dma((2, half)),
            dma((n_sp, n_tp)),
            dma((n_sp, n_tp)),
            dma((n_sp, n_tp)),
            dma((n_sp, n_tp)),
            dma((2, half + 1)),
            dma((2, half + 1)),
        ],
        compiler_params=pltpu.CompilerParams(
            collective_id=0, has_side_effects=True, vmem_limit_bytes=63 * 1024 * 1024
        ),
    )(normed, stream, meta, eg, eu, ed, sg, su, sd)


def route_table(routes, route_weights, experts_total, capacity):
    top_count = routes.shape[1]
    row_count = routes.shape[0]
    ids = routes.T
    experts = jnp.arange(experts_total, dtype=jnp.int32)
    named = ids[:, None, :] == experts[None, :, None]
    onehot = jnp.any(named, axis=0).astype(jnp.bfloat16)
    order = jnp.arange(row_count)
    earlier = (order[:, None] < order[None, :]).astype(jnp.bfloat16)
    before = jnp.dot(onehot, earlier, preferred_element_type=jnp.float32)
    slot = before + (experts * capacity).astype(jnp.float32)[:, None]
    slots = jnp.sum(jnp.where(named, slot[None], 0.0), axis=1)
    weights = route_weights.T
    gates = weights / jnp.sum(weights, axis=0, keepdims=True) * 2.5
    spare = jnp.zeros((META_ROWS - 2 * top_count, row_count), jnp.float32)
    return jnp.concatenate([slots, gates, spare], axis=0)


def body(
    out_gate,
    in_gate,
    conv_values,
    conv_taps,
    mix_gain,
    out_proj,
    residual,
    ffn_gain,
    routes,
    route_weights,
    shared_gate,
    shared_up,
    shared_down,
    expert_gate,
    expert_up,
    expert_down,
):
    mixed_in = in_gate.astype(jnp.float32) * conv_values.astype(jnp.float32)
    taps_count = conv_taps.shape[0]
    length = mixed_in.shape[0]
    earlier = from_behind(mixed_in[length - (taps_count - 1) :], "sp", 1)
    extended = jnp.concatenate([earlier, mixed_in], axis=0)
    filtered = conv_taps[0] * extended[0:length]
    for offset in range(1, taps_count):
        filtered = filtered + conv_taps[offset] * extended[offset : offset + length]
    conv_out = (out_gate.astype(jnp.float32) * filtered).astype(jnp.bfloat16)
    row_count = length // lax.axis_size("tp")
    token_rows = lax.all_to_all(conv_out, "tp", split_axis=0, concat_axis=1, tiled=True)
    mix_result = project_norm(token_rows, mix_gain, out_proj)
    stream = residual.astype(jnp.float32) + mix_result
    norm_inverse = lax.rsqrt(jnp.mean(stream * stream, axis=-1, keepdims=True) + 1e-06)
    normed = (stream * norm_inverse * ffn_gain).astype(jnp.bfloat16)
    experts_total = lax.axis_size("sp") * lax.axis_size("tp")
    top_count = routes.shape[1]
    capacity = max(2, 4 * row_count * top_count // (3 * experts_total))
    meta = route_table(routes, route_weights, experts_total, capacity)
    return routed_and_shared(
        normed, stream, meta, capacity, top_count,
        expert_gate, expert_up, expert_down, shared_gate, shared_up, shared_down,
    )


def solution(mesh):
    in_specs = (
        P("sp", "tp"),
        P("sp", "tp"),
        P("sp", "tp"),
        P(None, "tp"),
        P(),
        P(),
        P(("sp", "tp"), None),
        P(),
        P(("sp", "tp"), None),
        P(("sp", "tp"), None),
        P(),
        P(),
        P(),
        P(("sp", "tp"), None, None),
        P(("sp", "tp"), None, None),
        P(("sp", "tp"), None, None),
    )
    out_specs = P(("sp", "tp"), None)
    return jax.shard_map(body, mesh=mesh, in_specs=in_specs, out_specs=out_specs, check_vma=False)
```

```python
import functools

import jax
import jax.numpy as jnp
from jax import lax
from jax.experimental import pallas as pl
from jax.experimental.pallas import tpu as pltpu
from jax.sharding import PartitionSpec as P

MESH = pl.DeviceIdType.MESH
META_ROWS = 16
HALO = 16


def ffn(x, gate, up, down):
    g = jnp.dot(x, gate[...], preferred_element_type=jnp.float32)
    u = jnp.dot(x, up[...], preferred_element_type=jnp.float32)
    h = (g / (1.0 + jnp.exp(-g)) * u).astype(jnp.bfloat16)
    return jnp.dot(h, down[...], preferred_element_type=jnp.float32)


def experts_kernel(
    n_sp, n_tp, width_x, cap, top,
    og_hbm, ig_hbm, cv_hbm, taps, mix_gain, residual, ffn_gain, routes, route_weights,
    op_hbm, eg_hbm, eu_hbm, ed_hbm, sg_hbm, su_hbm, sd_hbm,
    out,
    og, ig, cv, conv_out, conv_in, normed, meta_own,
    gathered, metas, staged, arrived, results, returned,
    left_in, right_in, total,
    op, eg, eu, ed, sg, su, sd,
    w_sem, halo_send, halo_recv, conv_send, conv_recv,
    meta_send, meta_recv, ring_send, ring_recv,
    disp_send, disp_recv, ret_send, ret_recv, red_send, red_recv,
):
    sp = lax.axis_index("sp")
    tp = lax.axis_index("tp")
    half = n_sp // 2
    rows, width = normed.shape
    length = og.shape[0]
    mid = rows // 2
    group = n_tp * cap
    width_z = n_sp // width_x

    def place_of(index):
        x, z = lax.rem(index, width_x), lax.div(index, width_x)
        return x * width_z + z + lax.rem(x, 2) * (width_z - 1 - 2 * z)

    def index_of(place):
        x, zz = lax.div(place, width_z), lax.rem(place, width_z)
        return (zz + lax.rem(x, 2) * (width_z - 1 - 2 * zz)) * width_x + x

    place = place_of(sp)

    def ahead(distance):
        return index_of(lax.rem(place + distance, n_sp))

    right, left = ahead(1), ahead(n_sp - 1)

    def partner(j):
        return lax.rem(tp + j, n_tp)

    barrier = pltpu.get_barrier_semaphore()
    for d in range(1, n_sp):
        pl.semaphore_signal(barrier, inc=1, device_id=(ahead(d), tp), device_id_type=MESH)
    for j in range(1, n_tp):
        pl.semaphore_signal(barrier, inc=1, device_id=(sp, partner(j)), device_id_type=MESH)

    weights = [
        pltpu.make_async_copy(src, dst, w_sem.at[i])
        for i, (src, dst) in enumerate(
            ((ig_hbm, ig.at[pl.ds(HALO, length)]), (cv_hbm, cv.at[pl.ds(HALO, length)]),
             (og_hbm, og), (op_hbm, op), (sg_hbm, sg), (su_hbm, su), (sd_hbm, sd),
             (eg_hbm.at[0], eg), (eu_hbm.at[0], eu), (ed_hbm.at[0], ed))
        )
    ]
    for copy in weights:
        copy.start()
    pl.semaphore_wait(barrier, n_sp - 1 + n_tp - 1)

    def remote(src, dst, send, recv, device):
        return pltpu.make_async_remote_copy(
            src_ref=src, dst_ref=dst, send_sem=send, recv_sem=recv,
            device_id=device, device_id_type=MESH,
        )

    def meta_copy(d):
        return remote(meta_own, metas.at[d], meta_send.at[d], meta_recv.at[d], (ahead(d), tp))

    def ring_copy(s, way, src=None):
        device = (right if way == 0 else left, tp)
        dst = gathered.at[s + 1 if way == 0 else n_sp - s - 1]
        if src is None:
            src = gathered.at[s if way == 0 else lax.rem(n_sp - s, n_sp)]
        return remote(src, dst, ring_send.at[way, s], ring_recv.at[way, s], device)

    def ring_half(way):
        device = (right if way == 0 else left, tp)
        part = pl.ds(0 if way == 0 else mid, mid)
        s = half - 1
        src = gathered.at[s if way == 0 else n_sp - s, part]
        return remote(src, gathered.at[half, part], ring_send.at[way, s], ring_recv.at[way, s], device)

    def disp_copy(d, j):
        src = staged.at[d, pl.ds(pl.multiple_of(partner(j) * cap, cap), cap)]
        dst = arrived.at[d, pl.ds(pl.multiple_of(tp * cap, cap), cap)]
        return remote(src, dst, disp_send.at[d, j], disp_recv.at[d, j], (sp, partner(j)))

    def ret_copy(d, j):
        src = results.at[d, pl.ds(pl.multiple_of(partner(j) * cap, cap), cap)]
        dst = returned.at[d, pl.ds(pl.multiple_of(tp * cap, cap), cap)]
        return remote(src, dst, ret_send.at[d, j], ret_recv.at[d, j], (sp, partner(j)))

    def red_copy(s, way):
        device = (left if way == 0 else right, tp)
        src = gathered.at[s if way == 0 else n_sp - s]
        dst = (left_in if way == 0 else right_in).at[s - 1]
        return remote(src, dst, red_send.at[way, s], red_recv.at[way, s - 1], device)

    def red_half(way):
        device = (left if way == 0 else right, tp)
        part = pl.ds(0 if way == 0 else mid, mid)
        src = gathered.at[half, part]
        dst = (left_in if way == 0 else right_in).at[half - 1, part]
        return remote(src, dst, red_send.at[way, half], red_recv.at[way, half - 1], device)

    def halo_copy(i):
        src = (ig_hbm, cv_hbm)[i].at[pl.ds(length - HALO, HALO)]
        dst = (ig, cv)[i].at[pl.ds(0, HALO)]
        device = (lax.rem(sp + 1, n_sp), tp)
        return remote(src, dst, halo_send.at[i], halo_recv.at[i], device)

    def conv_copy(j):
        return remote(
            conv_out.at[j], conv_in.at[tp], conv_send.at[j], conv_recv.at[j], (sp, partner(j))
        )

    halo_copy(0).start()
    halo_copy(1).start()

    experts_total = n_sp * n_tp
    expert = lax.broadcasted_iota(jnp.int32, (experts_total, rows), 0)
    named = [routes[k : k + 1, :] == expert for k in range(top)]
    onehot = jnp.zeros((experts_total, rows), jnp.float32)
    for hit in named:
        onehot = jnp.where(hit, 1.0, onehot)
    earlier = lax.broadcasted_iota(jnp.int32, (rows, rows), 0) < lax.broadcasted_iota(
        jnp.int32, (rows, rows), 1
    )
    before = jnp.dot(
        onehot.astype(jnp.bfloat16),
        jnp.where(earlier, 1.0, 0.0).astype(jnp.bfloat16),
        preferred_element_type=jnp.float32,
    )
    slot = before + (expert * cap).astype(jnp.float32)
    meta_own[...] = jnp.zeros_like(meta_own)
    for k in range(top):
        meta_own[k : k + 1, :] = jnp.sum(jnp.where(named[k], slot, 0.0), axis=0, keepdims=True)
    weight = route_weights[...]
    meta_own[top : 2 * top, :] = weight / jnp.sum(weight, axis=0, keepdims=True) * 2.5

    for copy in weights[:3]:
        copy.wait()
    for d in range(1, n_sp):
        meta_copy(d).start()
    halo_copy(0).wait_recv()
    halo_copy(1).wait_recv()
    taps_count = taps.shape[0]
    for j in list(range(1, n_tp)) + [0]:
        start = pl.multiple_of(partner(j) * rows, rows)
        span = pl.ds(start, rows + HALO)
        mixed = ig[span].astype(jnp.float32) * cv[span].astype(jnp.float32)
        blank = jnp.where(sp * n_tp + partner(j) == 0, HALO, 0)
        at = lax.broadcasted_iota(jnp.int32, mixed.shape, 0)
        mixed = jnp.where(at >= blank, mixed, 0.0)
        base = HALO - (taps_count - 1)
        filtered = taps[0:1, :] * mixed[base : base + rows]
        for o in range(1, taps_count):
            filtered = filtered + taps[o : o + 1, :] * mixed[base + o : base + o + rows]
        value = (og[pl.ds(start, rows)].astype(jnp.float32) * filtered).astype(jnp.bfloat16)
        if j == 0:
            conv_in[tp] = value
        else:
            conv_out[j] = value
            conv_copy(j).start()
    weights[3].wait()
    for j in range(1, n_tp):
        conv_copy(j).wait_recv()
    squares = jnp.zeros((rows, 1), jnp.float32)
    product = jnp.zeros((rows, width), jnp.float32)
    part_width = conv_in.shape[2]
    for t in range(n_tp):
        value = conv_in[t].astype(jnp.float32)
        squares = squares + jnp.sum(value * value, axis=1, keepdims=True)
        product = product + jnp.dot(
            (value * mix_gain[t]).astype(jnp.bfloat16),
            op[t * part_width : (t + 1) * part_width, :],
            preferred_element_type=jnp.float32,
        )
    inverse = lax.rsqrt(squares / (n_tp * part_width) + 1e-06)
    stream = residual[...].astype(jnp.float32) + product * inverse
    power = jnp.mean(stream * stream, axis=1, keepdims=True)
    normed[...] = (stream * lax.rsqrt(power + 1e-06) * ffn_gain[...]).astype(jnp.bfloat16)
    total[...] = stream

    first_slot = (sp * group).astype(jnp.float32)

    def matches(meta, k):
        slots = lax.broadcasted_iota(jnp.int32, (group, rows), 0).astype(jnp.float32) + first_slot
        return slots == meta[k : k + 1, :]

    def dispatch(d, block, meta):
        pick = jnp.zeros((group, rows), jnp.float32)
        for k in range(top):
            pick = jnp.where(matches(meta, k), 1.0, pick)
        staged[d] = jnp.dot(
            pick.astype(jnp.bfloat16), block, preferred_element_type=jnp.float32
        ).astype(jnp.bfloat16)
        for j in range(1, n_tp):
            disp_copy(d, j).start()

    own = pl.ds(pl.multiple_of(tp * cap, cap), cap)

    def run_expert(d):
        for j in range(1, n_tp):
            disp_copy(d, j).wait_recv()
        arrived[d, own] = staged[d, own]
        results[d] = ffn(arrived[d], eg, eu, ed).astype(jnp.bfloat16)

    def combine(d, meta):
        for j in range(1, n_tp):
            ret_copy(d, j).wait_recv()
        returned[d, own] = results[d, own]
        mix = jnp.zeros((group, rows), jnp.float32)
        for k in range(top):
            mix = jnp.where(matches(meta, k), meta[top + k : top + k + 1, :], mix)
        return lax.dot_general(
            mix.astype(jnp.bfloat16), returned[d], (((0,), (0,)), ((), ())),
            preferred_element_type=jnp.float32,
        )

    ring_copy(0, 0, normed).start()
    ring_copy(0, 1, normed).start()
    dispatch(0, normed[...], meta_own[...])
    left_in[half - 1, mid:] = jnp.zeros((rows - mid, normed.shape[1]), jnp.bfloat16)
    right_in[half - 1, :mid] = jnp.zeros((mid, normed.shape[1]), jnp.bfloat16)
    for copy in weights[4:7]:
        copy.wait()
    total[...] += ffn(normed[...], sg, su, sd)
    for copy in weights[7:]:
        copy.wait()

    def gather_step(s, carry):
        ring_copy(s - 1, 0).wait_recv()
        ring_copy(s - 1, 1).wait_recv()

        @pl.when(s < half - 1)
        def _():
            ring_copy(s, 0).start()
            ring_copy(s, 1).start()

        @pl.when(s == half - 1)
        def _():
            ring_half(0).start()
            ring_half(1).start()

        def one(i, c):
            d = s + i * (n_sp - 2 * s)
            meta_copy(d).wait_recv()
            dispatch(d, gathered[d], metas[d])
            return c

        lax.fori_loop(0, 2, one, 0)

        @pl.when(s == 1)
        def _():
            run_expert(0)

        @pl.when(s > 1)
        def _():
            def two(i, c):
                run_expert(s - 1 + i * (n_sp - 2 * (s - 1)))
                return c

            lax.fori_loop(0, 2, two, 0)

        return carry

    lax.fori_loop(1, half, gather_step, 0)
    ring_half(0).wait_recv()
    ring_half(1).wait_recv()
    meta_copy(half).wait_recv()
    dispatch(half, gathered[half], metas[half])

    def give_back(d):
        for j in range(1, n_tp):
            ret_copy(d, j).start()

    def last(i, c):
        d = half - 1 + 2 * i - 3 * lax.div(i, 2)
        run_expert(d)
        give_back(d)
        return c

    lax.fori_loop(0, 3, last, 0)
    for s in range(half - 2, 0, -1):
        give_back(s)
        give_back(n_sp - s)
    give_back(0)

    for way in range(2):
        ring_copy(0, way, normed).wait_send()
        for s in range(1, half - 1):
            ring_copy(s, way).wait_send()
        ring_half(way).wait_send()
    part = combine(half, metas[half])
    gathered[half] = part.astype(jnp.bfloat16)
    red_half(0).start()
    red_half(1).start()

    def reduce_step(i, carry):
        s = half - 1 - i
        for way, (d, buf_in) in enumerate(((s, left_in), (n_sp - s, right_in))):
            part = combine(d, metas[d])

            @pl.when(s == half - 1)
            def _():
                red_half(way).wait_recv()

            @pl.when(s < half - 1)
            def _():
                red_copy(s + 1, way).wait_recv()

            gathered[d] = (part + buf_in[s].astype(jnp.float32)).astype(jnp.bfloat16)
            red_copy(s, way).start()
        return carry

    lax.fori_loop(0, half - 1, reduce_step, 0)
    part = combine(0, meta_own[...]) + total[...]
    for way, buf_in in enumerate((left_in, right_in)):
        red_copy(1, way).wait_recv()
        part = part + buf_in[0].astype(jnp.float32)
    out[...] = part.astype(out.dtype)

    for d in range(1, n_sp):
        meta_copy(d).wait_send()
    for j in range(1, n_tp):
        conv_copy(j).wait_send()
    for way in range(2):
        halo_copy(way).wait_send()
        red_half(way).wait_send()
        for s in range(1, half):
            red_copy(s, way).wait_send()

    def drain(d, c):
        for j in range(1, n_tp):
            disp_copy(d, j).wait_send()
            ret_copy(d, j).wait_send()
        return c

    lax.fori_loop(0, n_sp, drain, 0)


def body(
    out_gate,
    in_gate,
    conv_values,
    conv_taps,
    mix_gain,
    out_proj,
    residual,
    ffn_gain,
    routes,
    route_weights,
    shared_gate,
    shared_up,
    shared_down,
    expert_gate,
    expert_up,
    expert_down,
):
    n_sp, n_tp = lax.axis_size("sp"), lax.axis_size("tp")
    length, channels = in_gate.shape
    rows, width = residual.shape
    top = routes.shape[1]
    cap = max(2, 4 * rows * top // (3 * n_sp * n_tp))
    hidden, shared_hidden = expert_gate.shape[-1], shared_gate.shape[-1]
    half = n_sp // 2
    group = n_tp * cap
    width_x = max(1, n_tp // 2)
    if n_sp % width_x:
        width_x = 1
    bf, f32 = jnp.bfloat16, jnp.float32
    vmem = pl.BlockSpec(memory_space=pltpu.VMEM)
    anywhere = pl.BlockSpec(memory_space=pl.ANY)
    dma = pltpu.SemaphoreType.DMA
    return pl.pallas_call(
        functools.partial(experts_kernel, n_sp, n_tp, width_x, cap, top),
        out_shape=jax.ShapeDtypeStruct((rows, width), bf),
        in_specs=[anywhere] * 3 + [vmem] * 6 + [anywhere] * 7,
        out_specs=vmem,
        scratch_shapes=[
            pltpu.VMEM((length, channels), bf),
            pltpu.VMEM((length + HALO, channels), bf),
            pltpu.VMEM((length + HALO, channels), bf),
            pltpu.VMEM((n_tp, rows, channels), bf),
            pltpu.VMEM((n_tp, rows, channels), bf),
            pltpu.VMEM((rows, width), bf),
            pltpu.VMEM((META_ROWS, rows), f32),
            pltpu.VMEM((n_sp, rows, width), bf),
            pltpu.VMEM((n_sp, META_ROWS, rows), f32),
            pltpu.VMEM((n_sp, group, width), bf),
            pltpu.VMEM((n_sp, group, width), bf),
            pltpu.VMEM((n_sp, group, width), bf),
            pltpu.VMEM((n_sp, group, width), bf),
            pltpu.VMEM((half, rows, width), bf),
            pltpu.VMEM((half, rows, width), bf),
            pltpu.VMEM((rows, width), f32),
            pltpu.VMEM((n_tp * channels, width), bf),
            pltpu.VMEM((width, hidden), bf),
            pltpu.VMEM((width, hidden), bf),
            pltpu.VMEM((hidden, width), bf),
            pltpu.VMEM((width, shared_hidden), bf),
            pltpu.VMEM((width, shared_hidden), bf),
            pltpu.VMEM((shared_hidden, width), bf),
            dma((10,)),
            dma((2,)),
            dma((2,)),
            dma((n_tp,)),
            dma((n_tp,)),
            dma((n_sp,)),
            dma((n_sp,)),
            dma((2, half)),
            dma((2, half)),
            dma((n_sp, n_tp)),
            dma((n_sp, n_tp)),
            dma((n_sp, n_tp)),
            dma((n_sp, n_tp)),
            dma((2, half + 1)),
            dma((2, half + 1)),
        ],
        compiler_params=pltpu.CompilerParams(
            collective_id=0, has_side_effects=True, vmem_limit_bytes=63 * 1024 * 1024
        ),
    )(
        out_gate, in_gate, conv_values, conv_taps, mix_gain.reshape(n_tp, 1, channels),
        residual, ffn_gain.reshape(1, width), routes.T, route_weights.T,
        out_proj, expert_gate, expert_up, expert_down, shared_gate, shared_up, shared_down,
    )


def solution(mesh):
    in_specs = (
        P("sp", "tp"),
        P("sp", "tp"),
        P("sp", "tp"),
        P(None, "tp"),
        P(),
        P(),
        P(("sp", "tp"), None),
        P(),
        P(("sp", "tp"), None),
        P(("sp", "tp"), None),
        P(),
        P(),
        P(),
        P(("sp", "tp"), None, None),
        P(("sp", "tp"), None, None),
        P(("sp", "tp"), None, None),
    )
    out_specs = P(("sp", "tp"), None)
    return jax.shard_map(body, mesh=mesh, in_specs=in_specs, out_specs=out_specs, check_vma=False)
```
